512 devices in a mesh: sp: 128 (over z, x, core), tp: 4 (over y).
Axes of the slice: x: 4, y: 4, z: 16, core: 2. Of those that a mesh axis runs over, the one named last changes fastest.
Arguments:
- tokens: bfloat16 [49152, 2048], P('sp'), may hold values from -6 to 6
- doc_ids: int32 [49152], P('sp'), may hold values from 0 to 31, never falling along the last dimension, each value on 1 to 3072 neighbouring positions
- pre_gain: float32 [2, 2048], replicated, may hold values from 0.1 to 1.9
- value_proj: bfloat16 [2, 2048, 1024], P(None, 'sp', 'tp'), may hold values from -0.5 to 0.5
- gate_proj: bfloat16 [2, 2048, 1024], P(None, 'sp', 'tp'), may hold values from -0.5 to 0.5
- out_proj: bfloat16 [2, 1024, 2048], P(None, 'tp', 'sp'), may hold values from -0.1875 to 0.1875
- conv_taps: float32 [2, 31, 1024], P(None, None, 'tp'), may hold values from -2.2 to 2.2
- norm_gain: float32 [2, 1024], P(None, 'tp'), may hold values from 0.1 to 1.9
- norm_shift: float32 [2, 1024], P(None, 'tp'), may hold values from -3 to 3
Outputs:
- hidden: bfloat16 [49152, 2048], P('sp')
The draws below stay inside these ranges and needn't reach their ends.
Inputs may be any that keep to these rules, and one draw needn't show every extreme that they name: `doc_ids`: document numbers never fall along the sequence; each document has 1 to 3072 positions.
All inputs are finite; a program needn't handle non-finite values.
Results may differ from the reference program's by a relative error of at most 0.017.
Values may be sent and summed in bfloat16 or wider, within the bound.
A program may use at most 64 MiB of HBM per device.

```python
import math
import jax
import jax.numpy as jnp
import numpy as np
from jax import lax

D = 2048
C = 1024
KW = 31
LAYERS = 2
TOKENS = 49152
DOCS = 32
DOC_MOST = 3072
N_TP = 4


def draw_conv_taps(key, part):
    scale_key = jax.random.fold_in(key, 11)
    tap_key = jax.random.fold_in(key, 12)
    group_scale = jnp.exp(jax.random.uniform(scale_key, (8,), jnp.float32, jnp.log(0.25), jnp.log(4.0)))
    channel_scale = jnp.repeat(group_scale, C // 8)
    raw = jnp.clip(jax.random.normal(tap_key, (LAYERS, KW, C), jnp.float32), -3.0, 3.0)
    return raw * channel_scale[None, None, :] / jnp.sqrt(jnp.float32(KW))


def spiked(drawn, stream_key, source, target, parts, factor):
    owner, partner = [(jnp.arange(drawn.shape[dim]) // (drawn.shape[dim] // parts)).reshape([-1 if axis == dim else 1 for axis in range(drawn.ndim)]) for dim in (source, target)]
    chosen = jax.random.permutation(stream_key, parts)[partner]
    strong = (owner == chosen) | (owner == (partner + parts // 2) % parts)
    return jnp.where(strong, factor * drawn, drawn)


def levels(rng, dims, shards, smallest, high):
    factor_of, own = 1.0, jax.random.fold_in(rng, 6)
    for dim, parts in shards:
        heights = jnp.exp(jax.random.uniform(jax.random.fold_in(own, dim), (parts,), jnp.float32, smallest / len(shards), high / len(shards)))
        factor_of = factor_of * jnp.repeat(heights, dims[dim] // parts).reshape([-1 if axis == dim else 1 for axis in range(len(dims))])
    return factor_of


def length_profile(count, total, most, lean):
    portions = [(1 << 20) // math.isqrt(rank ** lean) + 1 for rank in range(2, count + 1)]
    rest, holding = total - most - (count - 1), [1] * (count - 1)
    while rest > 0:
        movable = [i for i in range(count - 1) if holding[i] < most]
        whole, remaining = sum([portions[i] for i in movable]), rest
        for i in movable:
            extra = min(most - holding[i], max(1, remaining * portions[i] // whole), rest)
            holding[i] = holding[i] + extra
            rest = rest - extra
    return np.array([most] + holding)


def ragged_sizes(own_key, number_of, total, limit, slope):
    if number_of == 2:
        one = jax.random.randint(own_key, (), max(1, total - limit), min(limit, total - 1) + 1)
        return jnp.stack([one, total - one])
    sizes = jnp.asarray(length_profile(number_of, total, limit, slope), jnp.int32)
    couples = (number_of - 1) // 2
    giver, receiver = sizes[1:1 + 2 * couples:2], sizes[2:2 + 2 * couples:2]
    margin = jnp.minimum(giver - 1, limit - receiver)
    passed = jax.random.randint(jax.random.fold_in(own_key, 1), (couples,), 0, 1 << 20) % (margin + 1)
    sizes = sizes.at[1:1 + 2 * couples:2].set(giver - passed).at[2:2 + 2 * couples:2].set(receiver + passed)
    return sizes[jax.random.permutation(jax.random.fold_in(own_key, 2), number_of)]


def scatter_about(rng, extent, scale, most, cuts=(), held_as=jnp.bfloat16):
    array = scale * jax.random.normal(rng, extent, jnp.float32)
    if cuts:
        array = array * levels(rng, extent, cuts, -0.22, 0.18)
    return jnp.clip(array, -most, most).astype(held_as)


def gaussian_with(rng, dims, scale, limit, cuts, heavy, dtype=jnp.bfloat16):
    array = scale * jax.random.normal(rng, dims, jnp.float32)
    if cuts:
        array = array * levels(rng, dims, cuts, -0.22, 0.18)
    return jnp.clip(spiked(array, jax.random.fold_in(rng, 3), *heavy), -limit, limit).astype(dtype)


def setup_inputs(seed: int = 0) -> dict:
    seeds = jax.random.split(jax.random.key(seed), 10)
    tokens = scatter_about(seeds[0], (TOKENS, D), 1.0, 6.0, ((0, 128),))
    doc_ids = jnp.searchsorted(jnp.cumsum(ragged_sizes(seeds[1], DOCS, TOKENS, DOC_MOST, 0)), jnp.arange(TOKENS), side="right").astype(jnp.int32)
    pre_gain = jnp.clip(1.0 + 0.18 * jax.random.normal(seeds[2], (LAYERS, D), jnp.float32), 0.1, 1.9)
    value_proj = gaussian_with(seeds[3], (LAYERS, D, C), D ** -0.5, 0.5, ((1, 128), (2, 4)), (1, 2, 128, 5.5))
    gate_proj = gaussian_with(seeds[4], (LAYERS, D, C), D ** -0.5, 0.5, ((1, 128), (2, 4)), (1, 2, 128, 5.5))
    out_proj = scatter_about(seeds[5], (LAYERS, C, D), C ** -0.5, 0.1875, ((1, 4), (2, 128)))
    conv_taps = draw_conv_taps(jax.random.fold_in(seeds[9], 71), 0)
    norm_gain = jnp.clip(1.0 + 0.18 * jax.random.normal(seeds[7], (LAYERS, C), jnp.float32), 0.1, 1.9)
    norm_shift = scatter_about(seeds[8], (LAYERS, C), 0.5, 3.0, ((1, 4),), jnp.float32)
    return dict(tokens=tokens, doc_ids=doc_ids, pre_gain=pre_gain, value_proj=value_proj, gate_proj=gate_proj, out_proj=out_proj, conv_taps=conv_taps, norm_gain=norm_gain, norm_shift=norm_shift)


epsilon = 1e-06

def reference(tokens, doc_ids, pre_gain, value_proj, gate_proj, out_proj, conv_taps, norm_gain, norm_shift):
    hidden = tokens
    padded_docs = jnp.concatenate([jnp.full((KW - 1,), -1, jnp.int32), doc_ids.astype(jnp.int32)])
    block_width = C // N_TP
    for layer_index in range(LAYERS):
        wide_state = hidden.astype(jnp.float32)
        scale = lax.rsqrt(lax.optimization_barrier(jnp.mean(wide_state * wide_state, axis=-1, keepdims=True)) + epsilon)
        normed = (wide_state * scale * pre_gain[layer_index]).astype(jnp.bfloat16)
        value_half = jnp.dot(normed, value_proj[layer_index], preferred_element_type=jnp.float32).astype(jnp.bfloat16)
        gate_half = jnp.dot(normed, gate_proj[layer_index], preferred_element_type=jnp.float32).astype(jnp.bfloat16)
        gated_rows = (value_half.astype(jnp.float32) * jax.nn.sigmoid(gate_half.astype(jnp.float32))).astype(jnp.bfloat16)
        padded = jnp.concatenate([jnp.zeros((KW - 1, C), jnp.bfloat16), gated_rows]).astype(jnp.float32)
        conv_out = jnp.zeros((TOKENS, C), jnp.float32)
        for offset in range(KW):
            first_row = KW - 1 - offset
            same_doc = (padded_docs[first_row:first_row + TOKENS] == doc_ids)[:, None]
            term = conv_taps[layer_index, offset][None, :] * padded[first_row:first_row + TOKENS]
            conv_out = conv_out + jnp.where(same_doc, term, jnp.float32(0.0))
        row_mean = lax.optimization_barrier(jnp.mean(conv_out, axis=-1, keepdims=True))
        row_var = lax.optimization_barrier(jnp.mean(jnp.square(conv_out - row_mean), axis=-1, keepdims=True))
        normalized = norm_gain[layer_index] * (conv_out - row_mean) * lax.rsqrt(row_var + epsilon) + norm_shift[layer_index]
        activated = jax.nn.silu(normalized).astype(jnp.bfloat16)
        total = jnp.zeros((TOKENS, D), jnp.float32)
        for block_index in range(N_TP):
            lower = block_index * block_width
            share = jnp.dot(activated[:, lower:lower + block_width], out_proj[layer_index, lower:lower + block_width], preferred_element_type=jnp.float32)
            total = total + share.astype(jnp.bfloat16).astype(jnp.float32)
        branch = total.astype(jnp.bfloat16)
        hidden = (hidden.astype(jnp.float32) + branch.astype(jnp.float32)).astype(jnp.bfloat16)
    return hidden
```

```python
import functools

import jax
import jax.numpy as jnp
from jax import lax
from jax.experimental import pallas as pl
from jax.experimental.pallas import tpu as pltpu
from jax.sharding import PartitionSpec as P

EPS = 1e-06
NZ, NX, NC, NY = 16, 4, 2, 4
ROWS, D, C, CB, KW, LAYERS = 384, 2048, 1024, 256, 31, 2
HALO = 32
RB = 128
NB = ROWS // RB
HB = RB // 2
F32, BF16 = jnp.float32, jnp.bfloat16
MESH = pl.DeviceIdType.MESH


def kernel(tok_hbm, docs_ref, gain_ref, v_ref, g_ref, o_ref, taps_ref, ng_ref, ns_ref, out_hbm,
           tok, normed, vg, ot, ag, gs, ge, dx, age, act,
           loc_sem, out_sem, vgx_s, vgx_r, oty_s, oty_r, gsy_s, gsy_r, dx_s, dx_r, halo_s, halo_r,
           vgz_s, vgu_r, vgd_r, otz_s, otu_r, otd_r, otx_s, oxu_r, oxd_r, oxb_r,
           rel_s, rel_r, pv_s, pv_r, po_s, po_r, ag_s, ag_r):
    sp = lax.axis_index("sp")
    y = lax.axis_index("tp")
    z = sp // 8
    x = lax.rem(sp // 2, 4)
    c = lax.rem(sp, 2)

    def at(zz, xx, cc):
        return {"sp": lax.rem(zz + NZ, NZ) * 8 + lax.rem(xx + NX, NX) * 2 + cc}

    def along_y(step):
        return {"tp": lax.rem(y + step + NY, NY)}

    z_up, z_down = at(z + 1, x, c), at(z - 1, x, c)
    x_up, x_down, x_far = at(z, x + 1, c), at(z, x - 1, c), at(z, x + 2, c)
    partner = at(z, x, 1 - c)
    sp_next = {"sp": lax.rem(sp + 1, 128)}
    sp_prev = {"sp": lax.rem(sp + 127, 128)}
    xp, xm, xf = lax.rem(x + 1, NX), lax.rem(x + 3, NX), lax.rem(x + 2, NX)

    def zi(v):
        return lax.rem(v + NZ, NZ)

    def rcopy(src, dst, ssem, rsem, dev):
        return pltpu.make_async_remote_copy(
            src_ref=src, dst_ref=dst, send_sem=ssem, recv_sem=rsem,
            device_id=dev, device_id_type=MESH)

    def push(ref, ssem, rsem, dev):
        rcopy(ref, ref, ssem, rsem, dev).start()

    def sent(ref, ssem):
        rcopy(ref, ref, ssem, ssem, partner).wait_send()

    def got(ref, rsem):
        rcopy(ref, ref, rsem, rsem, partner).wait_recv()

    tok_in = pltpu.make_async_copy(tok_hbm, tok, loc_sem)
    tok_in.start()

    for l in range(LAYERS):
        vg[l, z, x, c, :, 0:CB] = v_ref[l]
        vg[l, z, x, c, :, CB:2 * CB] = g_ref[l]
        ot[l, y, z, x, c] = jnp.transpose(o_ref[l].astype(F32)).astype(BF16)
    gs[y, 0:2, :] = ng_ref[...]
    gs[y, 2:4, :] = ns_ref[...]
    for i in range(3):
        row = jnp.broadcast_to(docs_ref[i:i + 1, :].astype(F32), (128, 128))
        dx[HALO + 128 * i:HALO + 128 * (i + 1), :] = jnp.transpose(row)

    barrier = pltpu.get_barrier_semaphore()
    peers = [z_up, z_down, x_up, x_down, x_far, partner, sp_next, sp_prev,
             along_y(1), along_y(-1), along_y(2)]
    for dev in peers:
        pl.semaphore_signal(barrier, inc=1, device_id=dev, device_id_type=MESH)
    pl.semaphore_wait(barrier, len(peers))

    mine = vg.at[:, z, x, c]
    for i, dev in enumerate((x_up, x_down, x_far)):
        push(mine, vgx_s.at[i], vgx_r.at[i], dev)
    own_o = ot.at[:, y, z, x, c]
    for i, dev in enumerate((along_y(1), along_y(-1), along_y(2))):
        push(own_o, oty_s.at[i], oty_r.at[i], dev)
    for i, dev in enumerate((along_y(1), along_y(-1), along_y(2))):
        push(gs.at[y], gsy_s.at[i], gsy_r.at[i], dev)
    dx_tail, dx_head = dx.at[pl.ds(ROWS, HALO)], dx.at[pl.ds(0, HALO)]
    dx_copy = rcopy(dx_tail, dx_head, dx_s, dx_r, sp_next)
    dx_copy.start()
    for i in range(3):
        got(mine, vgx_r.at[i])

    def vg_part(l, zc, sub):
        return vg.at[l, zc, pl.ds(2 * sub, 2), c]

    def ot_part(l, zc, xx):
        return ot.at[l, :, zc, xx, c]

    def vg_up(l, r, sub):
        push(vg_part(l, zi(z - r), sub), vgz_s.at[l], vgu_r.at[l, sub, r], z_up)

    def vg_down(l, r, sub):
        push(vg_part(l, zi(z + r), sub), vgz_s.at[l], vgd_r.at[l, sub, r], z_down)

    def vg_to_partner(l, zc):
        push(vg.at[l, zc, :, c], pv_s.at[l], pv_r.at[l], partner)

    def ot_up(l, r):
        push(ot_part(l, zi(z - r), x), otz_s.at[l], otu_r.at[l, r], z_up)

    def ot_down(l, r):
        push(ot_part(l, zi(z + r), x), otz_s.at[l], otd_r.at[l, r], z_down)

    def ot_along_x_u(l, r):
        part = ot_part(l, zi(z - r), x)
        push(part, otx_s.at[l], oxu_r.at[l, r], x_up)
        push(part, otx_s.at[l], oxb_r.at[l, 0], x_down)

    def ot_along_x_d(l, r):
        part = ot_part(l, zi(z + r), x)
        push(part, otx_s.at[l], oxd_r.at[l, r], x_down)
        push(part, otx_s.at[l], oxb_r.at[l, 1], x_up)

    def relay_u(l, r):
        part = ot_part(l, zi(z - r), xm)
        got(part, oxu_r.at[l, r])
        push(part, rel_s.at[l], rel_r.at[l, 0], x_up)

    def relay_d(l, r):
        part = ot_part(l, zi(z + r), xp)
        got(part, oxd_r.at[l, r])
        push(part, rel_s.at[l], rel_r.at[l, 1], x_down)

    def first_vg(l):
        for sub in range(2):
            vg_up(l, 0, sub)
            vg_down(l, 0, sub)
        vg_to_partner(l, z)

    def first_ot(l):
        ot_up(l, 0)
        ot_down(l, 0)
        ot_along_x_u(l, 0)

    def middle(l, r):
        for sub in range(2):
            got(vg_part(l, zi(z - r), sub), vgu_r.at[l, sub, r - 1])
            vg_up(l, r, sub)
            got(vg_part(l, zi(z + r), sub), vgd_r.at[l, sub, r - 1])
            vg_down(l, r, sub)
        got(ot_part(l, zi(z - r), x), otu_r.at[l, r - 1])
        ot_up(l, r)
        got(ot_part(l, zi(z + r), x), otd_r.at[l, r - 1])
        ot_down(l, r)
        vg_to_partner(l, zi(z - r))
        vg_to_partner(l, zi(z + r))
        ot_along_x_u(l, r)
        ot_along_x_d(l, r)

    def seventh(l):
        for sub in range(2):
            got(vg_part(l, zi(z - 7), sub), vgu_r.at[l, sub, 6])
            vg_up(l, 7, sub)
            got(vg_part(l, zi(z + 7), sub), vgd_r.at[l, sub, 6])
        got(ot_part(l, zi(z - 7), x), otu_r.at[l, 6])
        ot_up(l, 7)
        got(ot_part(l, zi(z + 7), x), otd_r.at[l, 6])
        vg_to_partner(l, zi(z - 7))
        vg_to_partner(l, zi(z + 7))
        ot_along_x_u(l, 7)
        ot_along_x_d(l, 7)

    def eighth(l):
        for sub in range(2):
            got(vg_part(l, zi(z - 8), sub), vgu_r.at[l, sub, 7])
        vg_to_partner(l, zi(z - 8))
        got(ot_part(l, zi(z - 8), x), otu_r.at[l, 7])
        ot_along_x_u(l, 8)
        push(ot.at[l, :, :, x, c], po_s.at[l], po_r.at[l], partner)

    def relays(l, r):
        relay_u(l, r)
        relay_d(l, r)

    def vg_ready(l):
        got(vg.at[l, :, :, 1 - c], pv_r.at[l])

    def ot_columns(l):
        got(ot.at[l, :, pl.ds(0, 9), xp, c], oxb_r.at[l, 0])
        got(ot.at[l, :, pl.ds(0, 7), xm, c], oxb_r.at[l, 1])
        push(ot.at[l, :, :, xp, c], po_s.at[l], po_r.at[l], partner)
        push(ot.at[l, :, :, xm, c], po_s.at[l], po_r.at[l], partner)
        got(ot.at[l, :, pl.ds(0, 9), xf, c], rel_r.at[l, 0])
        got(ot.at[l, :, pl.ds(0, 7), xf, c], rel_r.at[l, 1])
        push(ot.at[l, :, :, xf, c], po_s.at[l], po_r.at[l], partner)

    def ot_ready(l):
        got(ot.at[l, :, :, :, 1 - c], po_r.at[l])

    first_vg(0)
    for i in range(3):
        got(own_o, oty_r.at[i])
    first_ot(0)

    def normalize(l, start, count):
        wide = tok[pl.ds(start, count), :].astype(F32)
        scale = lax.rsqrt(jnp.mean(wide * wide, axis=-1, keepdims=True) + EPS)
        normed[pl.ds(start, count), :] = (wide * scale * gain_ref[l:l + 1, :]).astype(BF16)

    tok_in.wait()

    @pl.loop(0, ROWS // 32)
    def _(i):
        normalize(0, pl.multiple_of(i * 32, 32), 32)

    dx_copy.wait()
    dx[0:HALO, :] = jnp.where(sp == 0, -1.0, dx[0:HALO, :])
    for b in range(NB):
        here = dx[HALO + b * RB:HALO + (b + 1) * RB, :]
        total = jnp.zeros((RB, 128), F32)
        for j in range(1, KW):
            lo = HALO + b * RB - j
            total = total + jnp.where(dx[lo:lo + RB, :] == here, 1.0, 0.0)
        age[b * RB:(b + 1) * RB, :] = total

    middle(0, 1)
    relay_u(0, 0)

    @pl.loop(2, 7)
    def _(r):
        middle(0, r)
        relays(0, r - 1)

    seventh(0)
    relays(0, 6)
    eighth(0)
    first_vg(1)
    first_ot(1)

    def gate(l):
        @pl.loop(0, NB)
        def _(i):
            start = pl.multiple_of(i * RB, RB)
            both = jnp.dot(normed[pl.ds(start, RB), :], vg[l].reshape(D, 2 * CB),
                           preferred_element_type=F32)
            value = both[:, :CB].astype(BF16).astype(F32)
            gates = both[:, CB:].astype(BF16).astype(F32)
            gated = (value * jax.nn.sigmoid(gates)).astype(BF16).astype(F32)
            for h in range(2):
                ge[l, h, pl.ds(pl.multiple_of(start + HALO, 32), RB), :] = gated[:, 128 * h:128 * (h + 1)]

    def halo_copy(l):
        return rcopy(ge.at[l, :, pl.ds(ROWS, HALO)], ge.at[l, :, pl.ds(0, HALO)],
                     halo_s.at[l], halo_r.at[l], sp_next)

    def conv(l, b):
        for h in range(2):
            lo = HALO + b * RB
            old = age[b * RB:(b + 1) * RB, :]
            lanes = slice(128 * h, 128 * (h + 1))
            total = taps_ref[l, 0:1, lanes] * ge[l, h, lo:lo + RB, :]
            for j in range(1, KW):
                term = taps_ref[l, j:j + 1, lanes] * ge[l, h, lo - j:lo - j + RB, :]
                total = total + jnp.where(old >= j, term, 0.0)
            ag[l, y, b * RB:(b + 1) * RB, lanes] = total.astype(BF16)

    def half(l, who, b, k):
        return ag.at[l, who, pl.ds(b * RB + k * HB, HB)]

    def send_block(l, b):
        push(half(l, y, b, 0), ag_s.at[l], ag_r.at[l, b, 0], along_y(1))
        push(half(l, y, b, 1), ag_s.at[l], ag_r.at[l, b, 3], along_y(-1))
        push(half(l, y, b, 1), ag_s.at[l], ag_r.at[l, b, 1], along_y(1))
        push(half(l, y, b, 0), ag_s.at[l], ag_r.at[l, b, 2], along_y(-1))

    below, above, far = lax.rem(y + 3, NY), lax.rem(y + 1, NY), lax.rem(y + 2, NY)

    def relay_block(l, b):
        got(half(l, below, b, 0), ag_r.at[l, b, 0])
        push(half(l, below, b, 0), ag_s.at[l], ag_r.at[l, b, 4], along_y(1))
        got(half(l, above, b, 1), ag_r.at[l, b, 3])
        push(half(l, above, b, 1), ag_s.at[l], ag_r.at[l, b, 5], along_y(-1))

    def block_ready(l, b):
        got(half(l, below, b, 1), ag_r.at[l, b, 1])
        got(half(l, above, b, 0), ag_r.at[l, b, 2])
        got(half(l, far, b, 0), ag_r.at[l, b, 4])
        got(half(l, far, b, 1), ag_r.at[l, b, 5])

    def activate(l, b):
        @pl.loop(0, RB // 32)
        def _(i):
            rows = pl.ds(pl.multiple_of(b * RB + i * 32, 32), 32)
            parts = [ag[l, k, rows, :].astype(F32) for k in range(NY)]
            mean = sum(jnp.sum(p, axis=-1, keepdims=True) for p in parts) * (1.0 / C)
            parts = [p - mean for p in parts]
            var = sum(jnp.sum(p * p, axis=-1, keepdims=True) for p in parts) * (1.0 / C)
            scale = lax.rsqrt(var + EPS)
            for k in range(NY):
                n = gs[k, l:l + 1, :] * parts[k] * scale + gs[k, 2 + l:3 + l, :]
                act[k, pl.ds(pl.multiple_of(i * 32, 32), 32), :] = (n * jax.nn.sigmoid(n)).astype(BF16)

    def project(l, b):
        @pl.loop(0, 4)
        def _(n):
            total = jnp.zeros((RB, 512), F32)
            for k in range(NY):
                weights = ot[l, k, pl.ds(n * 4, 4)].reshape(512, CB)
                total = total + lax.dot_general(act[k], weights, (((1,), (1,)), ((), ())),
                                                preferred_element_type=F32)
            cols = pl.ds(pl.multiple_of(n * 512, 512), 512)
            rows = pl.ds(b * RB, RB)
            tok[rows, cols] = (tok[rows, cols].astype(F32)
                               + total.astype(BF16).astype(F32)).astype(BF16)

    order = tuple(reversed(range(NB)))

    def layer(l, steps):
        steps = list(steps)

        def step():
            if steps:
                steps.pop(0)()

        gate(l)
        copy = halo_copy(l)
        copy.start()
        step()
        for n, b in enumerate(order):
            if b == 0:
                copy.wait()
                ge[l, :, 0:HALO, :] = jnp.where(sp == 0, 0.0, ge[l, :, 0:HALO, :])
            conv(l, b)
            send_block(l, b)
            if n:
                relay_block(l, order[n - 1])
        step()
        relay_block(l, order[-1])
        step()
        for n, b in enumerate(order):
            block_ready(l, b)
            activate(l, b)
            if n == 0:
                ot_columns(l)
                ot_ready(l)
            project(l, b)
            if l + 1 < LAYERS:
                @pl.loop(0, RB // 32)
                def _(i):
                    normalize(l + 1, pl.multiple_of(b * RB + i * 32, 32), 32)
            else:
                out_copy(b).start()
            step()
        while steps:
            step()

    def out_copy(b):
        rows = pl.ds(b * RB, RB)
        return pltpu.make_async_copy(tok.at[rows], out_hbm.at[rows], out_sem.at[b])

    def later_step(r):
        def run():
            if r == 7:
                seventh(1)
            elif r == 8:
                eighth(1)
            else:
                middle(1, r)
            relay_u(1, r - 1)
            if r > 1:
                relay_d(1, r - 1)
            if r == 8:
                relay_u(1, 8)
        return run

    for i in range(3):
        got(gs.at[y], gsy_r.at[i])
    relays(0, 7)
    relay_u(0, 8)
    vg_ready(0)
    layer(0, [later_step(r) for r in range(1, 9)])
    vg_ready(1)
    layer(1, [])

    for b in range(NB):
        out_copy(b).wait()
    for i in range(3):
        sent(mine, vgx_s.at[i])
        sent(own_o, oty_s.at[i])
        sent(gs.at[y], gsy_s.at[i])
    for l in range(LAYERS):
        sent(vg.at[l, pl.ds(0, 15), :, c], vgz_s.at[l])
        sent(vg.at[l, :, :, c], pv_s.at[l])
        sent(ot.at[l, :, pl.ds(0, 15), x, c], otz_s.at[l])
        sent(ot.at[l, :, :, pl.ds(0, 2), c], otx_s.at[l])
        sent(ot.at[l, :, :, 0, c], rel_s.at[l])
        sent(ot.at[l, :, :, :, c], po_s.at[l])
        sent(ag.at[l, pl.ds(0, 3)], ag_s.at[l])


def on_device(tokens, doc_ids, pre_gain, value_proj, gate_proj, out_proj, conv_taps, norm_gain, norm_shift):
    vmem = pl.BlockSpec(memory_space=pltpu.VMEM)
    hbm = pl.BlockSpec(memory_space=pl.ANY)
    dma = pltpu.SemaphoreType.DMA
    L = LAYERS
    return pl.pallas_call(
        kernel,
        out_shape=jax.ShapeDtypeStruct((ROWS, D), BF16),
        in_specs=[hbm] + [vmem] * 8,
        out_specs=hbm,
        scratch_shapes=[
            pltpu.VMEM((ROWS, D), BF16),
            pltpu.VMEM((ROWS, D), BF16),
            pltpu.VMEM((L, NZ, NX, NC, 16, 2 * CB), BF16),
            pltpu.VMEM((L, NY, NZ, NX, NC, 16, CB), BF16),
            pltpu.VMEM((L, NY, ROWS, CB), BF16),
            pltpu.VMEM((NY, 8, CB), F32),
            pltpu.VMEM((L, 2, HALO + ROWS, 128), F32),
            pltpu.VMEM((HALO + ROWS, 128), F32),
            pltpu.VMEM((ROWS, 128), F32),
            pltpu.VMEM((NY, RB, CB), BF16),
            dma(()), dma((NB,)),
            dma((3,)), dma((3,)), dma((3,)), dma((3,)), dma((3,)), dma((3,)),
            dma(()), dma(()), dma((L,)), dma((L,)),
            dma((L,)), dma((L, 2, 8)), dma((L, 2, 7)),
            dma((L,)), dma((L, 8)), dma((L, 7)),
            dma((L,)), dma((L, 9)), dma((L, 8)), dma((L, 2)),
            dma((L,)), dma((L, 2)),
            dma((L,)), dma((L,)), dma((L,)), dma((L,)),
            dma((L,)), dma((L, NB, 6)),
        ],
        compiler_params=pltpu.CompilerParams(
            collective_id=0, has_side_effects=True, vmem_limit_bytes=48 * 1024 * 1024),
    )(tokens, doc_ids.reshape(3, 128), pre_gain, value_proj, gate_proj, out_proj,
      conv_taps, norm_gain, norm_shift)


def solution(mesh):
    return jax.shard_map(
        on_device,
        mesh=mesh,
        in_specs=(
            P("sp", None),
            P("sp"),
            P(),
            P(None, "sp", "tp"),
            P(None, "sp", "tp"),
            P(None, "tp", "sp"),
            P(None, None, "tp"),
            P(None, "tp"),
            P(None, "tp"),
        ),
        out_specs=P("sp", None),
        check_vma=False,
    )
```
